32 devices in a mesh: fs: 8 (over z, y), tp: 4 (over x, core).
Axes of the slice: x: 2, y: 2, z: 4, core: 2. Of those that a mesh axis runs over, the one named last changes fastest.
Arguments:
- tokens: bfloat16 [8192, 2048], P('fs'), may hold values from -6 to 6
- norm_gain: float32 [2048], replicated, may hold values from 0.1 to 1.9
- gate_weight: bfloat16 [2048, 5632], P('fs', 'tp'), may hold values from -0.125 to 0.125
- up_weight: bfloat16 [2048, 5632], P('fs', 'tp'), may hold values from -0.125 to 0.125
- down_weight: bfloat16 [5632, 2048], P('tp', 'fs'), may hold values from -0.078125 to 0.078125
Outputs:
- mixed: bfloat16 [8192, 2048], P(('fs', 'tp'))
The draws below stay inside these ranges and needn't reach their ends.
All inputs are finite; a program needn't handle non-finite values.
Results may differ from the reference program's by a relative error of at most 0.014.
Values may be sent and summed in bfloat16 or wider, within the bound.
A program may use at most 128 MiB of HBM per device.

```python
import jax
import jax.numpy as jnp
from jax import lax

D = 2048
FF = 5632
TOKENS = 8192
N_FS = 8
N_TP = 4


def block_scale(own_key, extent, cuts, low, high):
    loudness = 1.0
    for axis_at, blocks in cuts:
        heights = jax.random.uniform(jax.random.fold_in(jax.random.fold_in(own_key, 6), axis_at), (blocks,), jnp.float32, low / len(cuts), high / len(cuts))
        loudness = loudness * jnp.repeat(jnp.exp(heights), extent[axis_at] // blocks).reshape((-1,) + (1,) * (len(extent) - 1 - axis_at))
    return loudness


def gaussian(key, dims, spread, limit, shards=(), kind=jnp.bfloat16):
    values = jax.random.normal(key, dims, jnp.float32) * spread
    if len(shards) > 0:
        values = block_scale(key, dims, shards, -0.22, 0.18) * values
    return jnp.clip(values, min=-limit, max=limit).astype(kind)


def setup_inputs(seed: int = 0) -> dict:
    splits = jax.random.split(jax.random.key(seed), 6)
    tokens = gaussian(splits[0], (TOKENS, D), 1.0, 6.0, ((0, 8),))
    norm_gain = jnp.clip(1.0 + 0.18 * jax.random.normal(splits[1], (D,), jnp.float32), 0.1, 1.9)
    gate_weight = gaussian(splits[2], (D, FF), D ** -0.5, 0.125, ((0, 8), (1, 4)))
    up_weight = gaussian(splits[3], (D, FF), D ** -0.5, 0.125, ((0, 8), (1, 4)))
    down_weight = gaussian(splits[4], (FF, D), FF ** -0.5, 0.078125, ((0, 4), (1, 8)))
    return {"tokens": tokens, "norm_gain": norm_gain, "gate_weight": gate_weight, "up_weight": up_weight, "down_weight": down_weight}


def block_rows(xrows, norm_gain, gate_weight, up_weight, down_weight):
    xf = xrows.astype(jnp.float32)
    scale = lax.rsqrt(lax.optimization_barrier(jnp.mean(xf * xf, axis=-1, keepdims=True)) + 1e-06)
    normed = (xf * scale * norm_gain).astype(jnp.bfloat16)
    gate = jnp.dot(normed, gate_weight, preferred_element_type=jnp.float32)
    up = jnp.dot(normed, up_weight, preferred_element_type=jnp.float32)
    hidden = (jax.nn.silu(gate) * up).astype(jnp.bfloat16)
    width = FF // N_TP

    def add_block(total, index):
        start = (index * width).astype(jnp.int32)
        left = lax.dynamic_slice_in_dim(hidden, start, width, 1)
        right = lax.dynamic_slice_in_dim(down_weight, start, width, 0)
        part = jnp.dot(left, right, preferred_element_type=jnp.float32).astype(jnp.bfloat16)
        return (total + part.astype(jnp.float32), None)
    total, unused = lax.scan(add_block, jnp.zeros((xrows.shape[0], D), jnp.float32), jnp.arange(N_TP, dtype=jnp.int32))
    return total.astype(jnp.bfloat16)

def reference(tokens, norm_gain, gate_weight, up_weight, down_weight):
    blocks = tokens.reshape(N_FS, TOKENS // N_FS, D)
    result = lax.map(lambda rows: block_rows(rows, norm_gain, gate_weight, up_weight, down_weight), blocks)
    return result.reshape(TOKENS, D)
```

```python
import functools

import jax
import jax.numpy as jnp
from jax import lax
from jax.experimental import pallas as pl
from jax.experimental.pallas import tpu as pltpu
from jax.sharding import PartitionSpec as P

MESH = pl.DeviceIdType.MESH
CORES = 2
GATE, UP, DOWN = 0, 1, 2


def fs_grid(n):
    ny = 1
    while ny * ny * 4 <= n:
        ny *= 2
    return n // ny, ny


def flip(v, bits):
    bit = 1
    while bit <= bits:
        if bits & bit:
            v = v + bit - 2 * bit * lax.rem(lax.div(v, bit), 2)
        bit *= 2
    return v


def block_order(nz, ny):
    order = [(0, 0)]
    for r in range(1, nz):
        order += [(r, 0)] + [(r - 1, s) for s in range(1, ny)]
    return order + [(nz - 1, s) for s in range(1, ny)]


def kernel(
    nz, ny, nx, tile, tok, gain, gw, uw, dw, out,
    xr, wg, wu, wd, ag, au, hid, pb, xv, sv, av, bv,
    own_sem, tok_sem, tok_recv, z_sem, y_sem, c_sem, w_recv, x_sem, x_recv, a_sem, a_recv, b_sem, b_recv,
):
    fs, tp = lax.axis_index("fs"), lax.axis_index("tp")
    z, y = lax.div(fs, ny), lax.rem(fs, ny)
    x, c = lax.div(tp, CORES), lax.rem(tp, CORES)
    near, other = flip(z, 1), 1 - c
    prim = c == lax.rem(z, 2)
    second = c != lax.rem(z, 2)
    count, width = xr.shape
    pieces, rp, ff = wg.shape[0], wg.shape[3], wg.shape[4]
    rows_in, wide = gw.shape[0], wd.shape[3]
    fp = ff // pieces
    part = count // nx
    half = part // 2
    keep = part // CORES

    def dev(z, y, x, c):
        return (z * ny + y, x * CORES + c)

    def send(src, dst, sent, got, where):
        pltpu.make_async_remote_copy(src_ref=src, dst_ref=dst, send_sem=sent, recv_sem=got, device_id=where, device_id_type=MESH).start()

    def wait(ref, sem):
        pltpu.make_async_copy(ref, ref, sem).wait()

    def slot(m, i, r, s):
        if m == DOWN:
            return wd.at[r, s, pl.ds(i * fp, fp)]
        return (wg, wu)[m].at[i, r, s]

    def mine(m, i):
        if m == DOWN:
            return dw.at[pl.ds(i * fp, fp)]
        return (gw, uw)[m].at[pl.ds(i * rp, rp)]

    def to_z(m, i, r):
        send(mine(m, i), slot(m, i, r, 0), z_sem.at[m, r], w_recv.at[m, i, r, 0], dev(flip(z, r), y, x, c))

    def to_y(m, i, r, src):
        for s in range(1, ny):
            send(src, slot(m, i, r, s), y_sem.at[m, s], w_recv.at[m, i, r, s], dev(z, flip(y, s), x, c))

    def to_core(m, i, r, s, src):
        send(src, slot(m, i, r, s), c_sem.at[m], w_recv.at[m, i, r, s], dev(z, y, x, other))

    def local(m, i):
        return pltpu.make_async_copy(mine(m, i), slot(m, i, 0, 0), own_sem.at[m, i])

    barrier = pltpu.get_barrier_semaphore()

    def greet(where):
        pl.semaphore_signal(barrier, inc=1, device_id=where, device_id_type=MESH)

    for r in range(1, nz):
        greet(dev(flip(z, r), y, x, c))
    for t in range(1, nx):
        greet(dev(z, y, flip(x, t), c))
    greet(dev(z, y, x, other))

    @pl.when(prim)
    def _():
        for s in range(1, ny):
            greet(dev(z, flip(y, s), x, c))
        pl.semaphore_wait(barrier, nz + nx + ny - 2)

    @pl.when(second)
    def _():
        greet(dev(near, y, x, other))
        pl.semaphore_wait(barrier, nz + nx)

    first = x * part

    @pl.when(prim)
    def _():
        rows = pl.ds(first, half)
        send(tok.at[rows], xr.at[rows], tok_sem.at[0], tok_recv.at[0, 0], dev(near, y, x, c))
        pltpu.make_async_copy(tok, xr, tok_sem.at[nx]).start()
        for m in (GATE, UP):
            for i in range(pieces):
                local(m, i).start()
        for i in range(pieces):
            for m in (GATE, UP):
                to_y(m, i, 0, mine(m, i))
                for r in range(2, nz, 2):
                    to_z(m, i, r)
        for m in (GATE, UP):
            for i in range(pieces):
                to_core(m, i, 0, 0, mine(m, i))
        for i in range(pieces):
            local(DOWN, i).start()
            to_core(DOWN, i, 0, 0, mine(DOWN, i))
        wait(xr, tok_sem.at[nx])

    @pl.when(second)
    def _():
        rows = pl.ds(first + half, half)
        send(tok.at[rows], xr.at[rows], tok_sem.at[0], tok_recv.at[1, 0], dev(near, y, x, other))
        for i in range(pieces):
            for r in range(1, nz, 2):
                for m in (GATE, UP):
                    to_z(m, i, r)
        for h in range(2):
            rows = pl.ds(first + h * half, half)
            wait(xr.at[rows], tok_recv.at[h, 0])
            for t in range(1, nx):
                send(xr.at[rows], xr.at[rows], tok_sem.at[t], tok_recv.at[h, t], dev(z, y, flip(x, t), c))
        for t in range(1, nx):
            for h in range(2):
                rows = pl.ds(flip(x, t) * part + h * half, half)
                wait(xr.at[rows], tok_recv.at[h, t])
            wait(xr.at[pl.ds(first, part)], tok_sem.at[t])

    def normalize(t, carry):
        rows = pl.ds(pl.multiple_of(t * 32, 32), 32)
        xf = xr[rows, :].astype(jnp.float32)
        scale = lax.rsqrt(jnp.mean(xf * xf, axis=-1, keepdims=True) + 1e-06)
        xr[rows, :] = (xf * scale * gain[...]).astype(jnp.bfloat16)
        return carry

    lax.fori_loop(0, count // 32, normalize, 0)

    def columns(i, r, s):
        at = (flip(z, r) * ny + flip(y, s)) * rows_in + i * rp
        return pl.ds(pl.multiple_of(at, rp), rp)

    def accumulate(i, pair, begin, end):
        rs = (2 * pair, 2 * pair + 1)

        def step(t, carry):
            rows = pl.ds(pl.multiple_of(t * tile, tile), tile)
            left = jnp.concatenate([xr[rows, columns(i, r, s)] for r in rs for s in range(ny)], axis=1)
            both = []
            for w, acc in ((wg, ag), (wu, au)):
                right = w[i, rs[0] : rs[1] + 1].reshape(2 * ny * rp, ff)
                total = jnp.dot(left, right, preferred_element_type=jnp.float32)
                if not begin:
                    total = acc[rows, :] + total
                if not end:
                    acc[rows, :] = total
                both.append(total)
            if end:
                g, u = both
                hid[rows, :] = (g / (1.0 + jnp.exp(-g)) * u).astype(jnp.bfloat16)
            return carry

        lax.fori_loop(0, count // tile, step, 0)

    def take(m, i, r, s):
        if (r, s) == (0, 0):

            @pl.when(prim)
            def _():
                local(m, i).wait()

            @pl.when(second)
            def _():
                wait(slot(m, i, r, s), w_recv.at[m, i, r, s])

        else:
            wait(slot(m, i, r, s), w_recv.at[m, i, r, s])

            @pl.when(prim)
            def _():
                if s == 0:
                    to_y(m, i, r, slot(m, i, r, s))
                to_core(m, i, r, s, slot(m, i, r, s))

    pairs = nz // 2
    for i in range(pieces):
        for pair in range(pairs):
            for s in range(ny):
                for r in (2 * pair, 2 * pair + 1):
                    for m in (GATE, UP):
                        take(m, i, r, s)
            end = i == pieces - 1 and pair == pairs - 1
            if end:

                @pl.when(prim)
                def _():
                    for k in range(pieces):
                        to_y(DOWN, k, 0, mine(DOWN, k))
                        for r in range(2, nz, 2):
                            to_z(DOWN, k, r)

                @pl.when(second)
                def _():
                    for k in range(pieces):
                        for r in range(1, nz, 2):
                            to_z(DOWN, k, r)

            accumulate(i, pair, i == 0 and pair == 0, end)

    order = block_order(nz, ny)

    def at(r, s):
        return r * ny + s

    def partial(r, s):
        j = at(r, s)
        for i in range(pieces):
            take(DOWN, i, r, s)

        def step(t, carry):
            rows = pl.ds(pl.multiple_of(t * tile, tile), tile)
            pb[j, rows, :] = jnp.dot(hid[rows, :], wd[r, s], preferred_element_type=jnp.float32).astype(jnp.bfloat16)
            return carry

        lax.fori_loop(0, count // tile, step, 0)
        for t in range(1, nx):
            there = flip(x, t)
            send(pb.at[j, pl.ds(there * part, part)], xv.at[t - 1, j], x_sem.at[t], x_recv.at[t, j], dev(z, y, there, c))

    def gather_x(r, s):
        j = at(r, s)
        total = pb[j, pl.ds(pl.multiple_of(x * part, part), part), :].astype(jnp.float32)
        for t in range(1, nx):
            wait(xv.at[t - 1, j], x_recv.at[t, j])
            total = total + xv[t - 1, j].astype(jnp.float32)
        sv[j] = total.astype(jnp.bfloat16)

        @pl.when(prim)
        def _():
            send(sv.at[j, pl.ds(other * keep, keep)], av.at[j], a_sem, a_recv.at[j], dev(z, y, x, other))

        @pl.when(second)
        def _():
            there = at(r ^ 1, s)
            for k in range(CORES):
                send(sv.at[j, pl.ds(k * keep, keep)], bv.at[there], b_sem.at[k], b_recv.at[there], dev(near, y, x, k))

    def finish(r, s):
        j = at(r, s)
        to = pl.ds(pl.multiple_of((flip(z, r) * ny + flip(y, s)) * wide, wide), wide)
        wait(bv.at[j], b_recv.at[j])

        @pl.when(prim)
        def _():
            a = sv[j, pl.ds(pl.multiple_of(c * keep, keep), keep), :].astype(jnp.float32)
            out[:, to] = (a + bv[j].astype(jnp.float32)).astype(jnp.bfloat16)

        @pl.when(second)
        def _():
            wait(av.at[j], a_recv.at[j])
            out[:, to] = (av[j].astype(jnp.float32) + bv[j].astype(jnp.float32)).astype(jnp.bfloat16)

    lag, late = 3, 6
    for n in range(len(order) + late):
        if n < len(order):
            partial(*order[n])
        if 0 <= n - lag < len(order):
            gather_x(*order[n - lag])
        if 0 <= n - late < len(order):
            finish(*order[n - late])

    wait(xr.at[pl.ds(0, half)], tok_sem.at[0])
    for t in range(1, nx):
        wait(xv.at[t - 1], x_sem.at[t])

    def block(m):
        return wd.at[0, 0] if m == DOWN else (wg, wu)[m].at[:, 0, 0]

    @pl.when(prim)
    def _():
        for m, whole, line in ((GATE, wg, wg.at[:, :, 0]), (UP, wu, wu.at[:, :, 0]), (DOWN, wd, wd.at[:, 0])):
            for r in range(2, nz, 2):
                wait(block(m), z_sem.at[m, r])
            for s in range(1, ny):
                wait(line, y_sem.at[m, s])
            wait(whole, c_sem.at[m])
        wait(av, a_sem)

    @pl.when(second)
    def _():
        for m in (GATE, UP, DOWN):
            for r in range(1, nz, 2):
                wait(block(m), z_sem.at[m, r])
        for k in range(CORES):
            wait(bv, b_sem.at[k])


def make_per_device(n, n_tp):
    nz, ny = fs_grid(n)
    nx = n_tp // CORES

    def per_device(tokens, norm_gain, gate_weight, up_weight, down_weight):
        count, width = tokens.shape
        rows, ff = gate_weight.shape
        wide = down_weight.shape[1]
        pieces = max(rows // 128, 1)
        keep = count // n_tp
        part = count // nx
        tile = min(256, count)
        bf16, f32 = jnp.bfloat16, jnp.float32
        dma = pltpu.SemaphoreType.DMA
        vmem = pl.BlockSpec(memory_space=pltpu.VMEM)
        hbm = pl.BlockSpec(memory_space=pl.ANY)
        return pl.pallas_call(
            functools.partial(kernel, nz, ny, nx, tile),
            name="gated_block",
            out_shape=jax.ShapeDtypeStruct((keep, width), bf16),
            in_specs=[hbm, vmem, hbm, hbm, hbm],
            out_specs=vmem,
            scratch_shapes=[
                pltpu.VMEM((count, width), bf16),
                pltpu.VMEM((pieces, nz, ny, rows // pieces, ff), bf16),
                pltpu.VMEM((pieces, nz, ny, rows // pieces, ff), bf16),
                pltpu.VMEM((nz, ny, ff, wide), bf16),
                pltpu.VMEM((count, ff), f32),
                pltpu.VMEM((count, ff), f32),
                pltpu.VMEM((count, ff), bf16),
                pltpu.VMEM((n, count, wide), bf16),
                pltpu.VMEM((nx - 1, n, part, wide), bf16),
                pltpu.VMEM((n, part, wide), bf16),
                pltpu.VMEM((n, keep, wide), bf16),
                pltpu.VMEM((n, keep, wide), bf16),
                dma((3, pieces)),
                dma((nx + 1,)),
                dma((2, nx)),
                dma((3, nz)),
                dma((3, ny)),
                dma((3,)),
                dma((3, pieces, nz, ny)),
                dma((nx,)),
                dma((nx, n)),
                dma,
                dma((n,)),
                dma((CORES,)),
                dma((n,)),
            ],
            compiler_params=pltpu.CompilerParams(collective_id=0, has_side_effects=True, vmem_limit_bytes=67043328),
        )(tokens, norm_gain.reshape(1, width), gate_weight, up_weight, down_weight)

    return per_device


def solution(mesh):
    placed = (P("fs", None), P(), P("fs", "tp"), P("fs", "tp"), P("tp", "fs"))
    return jax.shard_map(
        make_per_device(mesh.shape["fs"], mesh.shape["tp"]),
        mesh=mesh, in_specs=placed, out_specs=P(("fs", "tp"), None), check_vma=False,
    )
```

```python
import functools

import jax
import jax.numpy as jnp
from jax import lax
from jax.experimental import pallas as pl
from jax.experimental.pallas import tpu as pltpu
from jax.sharding import PartitionSpec as P

MESH = pl.DeviceIdType.MESH
CORES = 2
GATE, UP, DOWN = 0, 1, 2


def fs_grid(n):
    ny = 1
    while ny * ny * 4 <= n:
        ny *= 2
    return n // ny, ny


def flip(v, bits):
    bit = 1
    while bit <= bits:
        if bits & bit:
            v = v + bit - 2 * bit * lax.rem(lax.div(v, bit), 2)
        bit *= 2
    return v


def inner(z):
    return lax.rem(lax.rem(z, 2) + lax.rem(lax.div(z, 2), 2), 2)


def swap_last(v, on):
    return v + on * (1 - 2 * lax.rem(v, 2))


def kernel(
    nz, ny, nx, tile, tok, gain, gw, uw, dw, out,
    xr, wg, wu, wd, ag, au, hid, pb, xv, sv, av, bv,
    own_sem, tok_sem, tok_recv, z_sem, y_sem, c_sem, w_recv, x_sem, x_recv, a_sem, a_recv, b_sem, b_recv,
):
    fs, tp = lax.axis_index("fs"), lax.axis_index("tp")
    z, y = lax.div(fs, ny), lax.rem(fs, ny)
    x, c = lax.div(tp, CORES), lax.rem(tp, CORES)
    near, other = flip(z, 1), 1 - c
    prim = c == lax.rem(z, 2)
    second = c != lax.rem(z, 2)
    count, width = xr.shape
    pieces, rp, ff = wg.shape[1], wg.shape[3], wg.shape[4]
    rows_in, wide = gw.shape[0], wd.shape[3]
    fp = ff // pieces
    part = count // nx
    chunks = tok_recv.shape[0]
    chunk = part // chunks
    keep = part // CORES
    scope = jax.named_scope

    def dev(z, y, x, c):
        return (z * ny + y, x * CORES + c)

    def send(src, dst, sent, got, where):
        pltpu.make_async_remote_copy(src_ref=src, dst_ref=dst, send_sem=sent, recv_sem=got, device_id=where, device_id_type=MESH).start()

    def wait(ref, sem):
        pltpu.make_async_copy(ref, ref, sem).wait()

    inside = inner(z)

    def pick(edge, middle):
        if isinstance(edge, int) and edge == middle:
            return edge
        return edge + inside * (middle - edge)

    def source(q):
        if isinstance(q, tuple):
            return pick(source(q[0]), source(q[1]))
        there = flip(z, q)
        return swap_last(there, inside) if q > 1 else there

    def number(v):
        return pick(*v) if isinstance(v, tuple) else v

    def slot(m, i, q, s):
        i, q = number(i), number(q)
        if m == DOWN:
            return wd.at[q, s, pl.ds(i * fp, fp)]
        return (wg, wu)[m].at[q, i, s]

    def mine(m, i):
        if m == DOWN:
            return dw.at[pl.ds(i * fp, fp)]
        return (gw, uw)[m].at[pl.ds(i * rp, rp)]

    def to_z(m, i, r):
        there = flip(z, r)
        q = r if r < 2 else swap_last(r, inner(there))
        send(mine(m, i), slot(m, i, q, 0), z_sem.at[m, r], w_recv.at[m, i, q, 0], dev(there, y, x, c))

    def to_y(m, i, q, src):
        for s in range(1, ny):
            send(src, slot(m, i, q, s), y_sem.at[m, s], w_recv.at[m, number(i), number(q), s], dev(z, flip(y, s), x, c))

    def to_core(m, i, q, s, src):
        send(src, slot(m, i, q, s), c_sem.at[m], w_recv.at[m, number(i), number(q), s], dev(z, y, x, other))

    def local(m, i):
        return pltpu.make_async_copy(mine(m, i), slot(m, i, 0, 0), own_sem.at[m, i])

    barrier = pltpu.get_barrier_semaphore()

    def greet(where):
        pl.semaphore_signal(barrier, inc=1, device_id=where, device_id_type=MESH)

    for r in range(1, nz):
        greet(dev(flip(z, r), y, x, c))
    for t in range(1, nx):
        greet(dev(z, y, flip(x, t), c))
    greet(dev(z, y, x, other))

    @pl.when(prim)
    def _():
        for s in range(1, ny):
            greet(dev(z, flip(y, s), x, c))
        pltpu.make_async_copy(tok, xr, tok_sem.at[nx]).start()
        for i in range(pieces):
            for m in (GATE, UP, DOWN):
                local(m, i).start()
        with scope("barrier"):
            pl.semaphore_wait(barrier, nz + nx + ny - 2)

    @pl.when(second)
    def _():
        greet(dev(near, y, x, other))
        with scope("barrier"):
            pl.semaphore_wait(barrier, nz + nx)

    def token_rows(x, k):
        return pl.ds(x * part + k * chunk, chunk)

    def to_near(k, core):
        rows = token_rows(x, k)
        send(tok.at[rows], xr.at[rows], tok_sem.at[0], tok_recv.at[k, 0], dev(near, y, x, core))

    @pl.when(prim)
    def _():
        for k in range(0, chunks, 2):
            to_near(k, c)
        for i in range(pieces):
            for m in (GATE, UP):
                to_y(m, i, 0, mine(m, i))
                for r in range(2, nz, 2):
                    to_z(m, i, r)
        for m in (GATE, UP, DOWN):
            for i in range(pieces):
                if m == DOWN:
                    to_y(m, i, 0, mine(m, i))
                to_core(m, i, 0, 0, mine(m, i))
        with scope("tokens"):
            wait(xr, tok_sem.at[nx])

    @pl.when(second)
    def _():
        for k in range(1, chunks, 2):
            to_near(k, other)
        for r in range(1, nz, 2):
            for i in range(pieces):
                for m in (GATE, UP):
                    to_z(m, i, r)

        @pl.when(inner(z) == 1)
        def _():
            for i in range(pieces):
                for r in range(3, nz, 2):
                    to_z(DOWN, i, r)

        for k in range(chunks):
            rows = token_rows(x, k)
            with scope(f"tokens#k={k}"):
                wait(xr.at[rows], tok_recv.at[k, 0])
            for t in range(1, nx):
                send(xr.at[rows], xr.at[rows], tok_sem.at[t], tok_recv.at[k, t], dev(z, y, flip(x, t), c))
        with scope("tokens#x"):
            for t in range(1, nx):
                for k in range(chunks):
                    rows = token_rows(flip(x, t), k)
                    wait(xr.at[rows], tok_recv.at[k, t])
                wait(xr.at[pl.ds(x * part, part)], tok_sem.at[t])

    def normalize(t, carry):
        rows = pl.ds(pl.multiple_of(t * 32, 32), 32)
        xf = xr[rows, :].astype(jnp.float32)
        scale = lax.rsqrt(jnp.mean(xf * xf, axis=-1, keepdims=True) + 1e-06)
        xr[rows, :] = (xf * scale * gain[...]).astype(jnp.bfloat16)
        return carry

    with scope("normalize"):
        lax.fori_loop(0, count // 32, normalize, 0)

    def columns(q, i, s):
        at = (source(q) * ny + flip(y, s)) * rows_in + number(i) * rp
        return pl.ds(pl.multiple_of(at, rp), rp)

    def accumulate(group, begin=False, end=False):
        def step(t, carry):
            rows = pl.ds(pl.multiple_of(t * tile, tile), tile)
            left = jnp.concatenate([xr[rows, columns(q, i, s)] for q, i in group for s in range(ny)], axis=1)
            both = []
            for w, acc in ((wg, ag), (wu, au)):
                right = jnp.concatenate([w[number(q), number(i)].reshape(ny * rp, ff) for q, i in group], axis=0)
                total = jnp.dot(left, right, preferred_element_type=jnp.float32)
                if not begin:
                    total = acc[rows, :] + total
                if not end:
                    acc[rows, :] = total
                both.append(total)
            if end:
                g, u = both
                hid[rows, :] = (g / (1.0 + jnp.exp(-g)) * u).astype(jnp.bfloat16)
            return carry

        with scope("acc#" + "#".join(f"{q}={i}" for q, i in group)):
            lax.fori_loop(0, count // tile, step, 0)

    def take(m, i, q, s):
        if (q, s) == (0, 0):

            @pl.when(prim)
            def _():
                local(m, i).wait()

            @pl.when(second)
            def _():
                wait(slot(m, i, q, s), w_recv.at[m, number(i), number(q), s])

        else:
            with scope(f"take#m={m}#i={i}#q={q}#s={s}".replace(" ", "")):
                wait(slot(m, i, q, s), w_recv.at[m, number(i), number(q), s])

            @pl.when(prim)
            def _():
                if s == 0:
                    to_y(m, i, q, slot(m, i, q, s))
                to_core(m, i, q, s, slot(m, i, q, s))

    def take_both(i, q, rows):
        for s in rows:
            for m in (GATE, UP):
                take(m, i, q, s)

    def take_down(q, rows):
        for s in rows:
            for i in range(pieces):
                take(DOWN, i, q, s)

    here, away = range(1), range(1, ny)
    early, late = list(range(2, nz, 2)), [1] + list(range(3, nz, 2))
    every = range(pieces)
    for i in every:
        take_both(i, 0, range(ny))
    accumulate([(0, i) for i in every], begin=True)
    steps = [
        ((q0, q1), (i0, i1))
        for (q0, i0), (q1, i1) in zip([(q, i) for q in late for i in every], [(q, i) for i in every for q in late])
    ]

    def pass_on(n):
        if n < len(steps):
            q, i = steps[n]
            take_both(i, q, here)

    def down_to_z():
        @pl.when(prim)
        def _():
            for k in every:
                for r in range(2, nz, 2):
                    to_z(DOWN, k, r)

        @pl.when(second)
        def _():
            for k in every:
                to_z(DOWN, k, 1)

            @pl.when(inside == 0)
            def _():
                for k in every:
                    for r in range(3, nz, 2):
                        to_z(DOWN, k, r)

    for q in early:
        for i in every:
            take_both(i, q, here)
    pass_on(0)
    for q in early:
        for i in every:
            take_both(i, q, away)
    pass_on(1)
    for q in early:
        accumulate([(q, k) for k in every])
    pass_on(2)
    group = []
    for n, (q, i) in enumerate(steps):
        last = n == len(steps) - 1
        take_both(i, q, away)
        pass_on(n + 3)
        if n + 4 == max(len(steps), 4):
            down_to_z()
        group.append((q, i))
        if last or n == len(steps) - 2 or n % 2:
            accumulate(group, end=last)
            group = []

    def at(q, s):
        return q * ny + s

    def partial(q, s):
        j = at(q, s)

        def step(t, carry):
            rows = pl.ds(pl.multiple_of(t * tile, tile), tile)
            pb[j, rows, :] = jnp.dot(hid[rows, :], wd[q, s], preferred_element_type=jnp.float32).astype(jnp.bfloat16)
            return carry

        with scope(f"part#q={q}#s={s}"):
            lax.fori_loop(0, count // tile, step, 0)
        for t in range(1, nx):
            there = flip(x, t)
            send(pb.at[j, pl.ds(there * part, part)], xv.at[t - 1, j], x_sem.at[t], x_recv.at[t, j], dev(z, y, there, c))

    def gather_x(q, s):
        j = at(q, s)
        total = pb[j, pl.ds(pl.multiple_of(x * part, part), part), :].astype(jnp.float32)
        for t in range(1, nx):
            with scope(f"xwait#q={q}#s={s}"):
                wait(xv.at[t - 1, j], x_recv.at[t, j])
            total = total + xv[t - 1, j].astype(jnp.float32)
        sv[j] = total.astype(jnp.bfloat16)

        @pl.when(prim)
        def _():
            send(sv.at[j, pl.ds(other * keep, keep)], av.at[j], a_sem, a_recv.at[j], dev(z, y, x, other))

        @pl.when(second)
        def _():
            there = at(1 - q if q < 2 else q, s)
            for k in range(CORES):
                send(sv.at[j, pl.ds(k * keep, keep)], bv.at[there], b_sem.at[k], b_recv.at[there], dev(near, y, x, k))

    def finish(q, s):
        j = at(q, s)
        to = pl.ds(pl.multiple_of((source(q) * ny + flip(y, s)) * wide, wide), wide)
        with scope(f"bwait#q={q}#s={s}"):
            wait(bv.at[j], b_recv.at[j])

        @pl.when(prim)
        def _():
            a = sv[j, pl.ds(pl.multiple_of(c * keep, keep), keep), :].astype(jnp.float32)
            out[:, to] = (a + bv[j].astype(jnp.float32)).astype(jnp.bfloat16)

        @pl.when(second)
        def _():
            wait(av.at[j], a_recv.at[j])
            out[:, to] = (av[j].astype(jnp.float32) + bv[j].astype(jnp.float32)).astype(jnp.bfloat16)

    order = [(0, s) for s in range(ny)]
    for q in early:
        order += [(q, 0), (1, 0)] if q == 2 else [(q, 0)]
    if not early:
        order += [(1, 0)]
    for q in early:
        order += [(q, s) for s in away] + ([(1, s) for s in away] if q == 2 else [])
    if not early:
        order += [(1, s) for s in away]
    for q in late[1:]:
        order += [(q, 0)]
    for q in late[1:]:
        order += [(q, s) for s in away]
    ahead, lag, behind = 1, 3, 5
    finishes = {}
    for n, (q, s) in enumerate(order):
        n = max(n, order.index((1 - q if q < 2 else q, s)))
        finishes.setdefault(n + behind, []).append((q, s))
    for n in range(-ahead, len(order) + behind):
        if n + ahead < len(order):
            q, s = order[n + ahead]
            take_down(q, range(s, s + 1))
        if 0 <= n < len(order):
            partial(*order[n])
        if 0 <= n - lag < len(order):
            gather_x(*order[n - lag])
        for q, s in finishes.get(n, ()):
            finish(q, s)

    wait(xr.at[pl.ds(0, part // 2)], tok_sem.at[0])
    for t in range(1, nx):
        wait(xv.at[t - 1], x_sem.at[t])

    def block(m):
        return wd.at[0, 0] if m == DOWN else (wg, wu)[m].at[0, :, 0]

    @pl.when(prim)
    def _():
        for m, whole, line in ((GATE, wg, wg.at[:, :, 0]), (UP, wu, wu.at[:, :, 0]), (DOWN, wd, wd.at[:, 0])):
            for r in range(2, nz, 2):
                wait(block(m), z_sem.at[m, r])
            for s in range(1, ny):
                wait(line, y_sem.at[m, s])
            wait(whole, c_sem.at[m])
        wait(av, a_sem)

    @pl.when(second)
    def _():
        for m in (GATE, UP, DOWN):
            for r in range(1, nz, 2):
                wait(block(m), z_sem.at[m, r])
        for k in range(CORES):
            wait(bv, b_sem.at[k])


def make_per_device(n, n_tp):
    nz, ny = fs_grid(n)
    nx = n_tp // CORES

    def per_device(tokens, norm_gain, gate_weight, up_weight, down_weight):
        count, width = tokens.shape
        rows, ff = gate_weight.shape
        wide = down_weight.shape[1]
        pieces = max(rows // 128, 1)
        keep = count // n_tp
        part = count // nx
        chunks = 8
        tile = min(256, count)
        bf16, f32 = jnp.bfloat16, jnp.float32
        dma = pltpu.SemaphoreType.DMA
        vmem = pl.BlockSpec(memory_space=pltpu.VMEM)
        hbm = pl.BlockSpec(memory_space=pl.ANY)
        return pl.pallas_call(
            functools.partial(kernel, nz, ny, nx, tile),
            name="gated_block",
            out_shape=jax.ShapeDtypeStruct((keep, width), bf16),
            in_specs=[hbm, vmem, hbm, hbm, hbm],
            out_specs=vmem,
            scratch_shapes=[
                pltpu.VMEM((count, width), bf16),
                pltpu.VMEM((nz, pieces, ny, rows // pieces, ff), bf16),
                pltpu.VMEM((nz, pieces, ny, rows // pieces, ff), bf16),
                pltpu.VMEM((nz, ny, ff, wide), bf16),
                pltpu.VMEM((count, ff), f32),
                pltpu.VMEM((count, ff), f32),
                pltpu.VMEM((count, ff), bf16),
                pltpu.VMEM((n, count, wide), bf16),
                pltpu.VMEM((nx - 1, n, part, wide), bf16),
                pltpu.VMEM((n, part, wide), bf16),
                pltpu.VMEM((n, keep, wide), bf16),
                pltpu.VMEM((n, keep, wide), bf16),
                dma((3, pieces)),
                dma((nx + 1,)),
                dma((chunks, nx)),
                dma((3, nz)),
                dma((3, ny)),
                dma((3,)),
                dma((3, pieces, nz, ny)),
                dma((nx,)),
                dma((nx, n)),
                dma,
                dma((n,)),
                dma((CORES,)),
                dma((n,)),
            ],
            compiler_params=pltpu.CompilerParams(collective_id=0, has_side_effects=True, vmem_limit_bytes=67043328),
        )(tokens, norm_gain.reshape(1, width), gate_weight, up_weight, down_weight)

    return per_device


def solution(mesh):
    placed = (P("fs", None), P(), P("fs", "tp"), P("fs", "tp"), P("tp", "fs"))
    return jax.shard_map(
        make_per_device(mesh.shape["fs"], mesh.shape["tp"]),
        mesh=mesh, in_specs=placed, out_specs=P(("fs", "tp"), None), check_vma=False,
    )
```

```python
import functools

import jax
import jax.numpy as jnp
from jax import lax
from jax.experimental import pallas as pl
from jax.experimental.pallas import tpu as pltpu
from jax.sharding import PartitionSpec as P

MESH = pl.DeviceIdType.MESH
CORES = 2
GATE, UP, DOWN = 0, 1, 2


def fs_grid(n):
    ny = 1
    while ny * ny * 4 <= n:
        ny *= 2
    return n // ny, ny


def flip(v, bits):
    bit = 1
    while bit <= bits:
        if bits & bit:
            v = v + bit - 2 * bit * lax.rem(lax.div(v, bit), 2)
        bit *= 2
    return v


def inner(z):
    return lax.rem(lax.rem(z, 2) + lax.rem(lax.div(z, 2), 2), 2)


def swap_last(v, on):
    return v + on * (1 - 2 * lax.rem(v, 2))


def kernel(
    nz, ny, nx, tile, tok, gain, gw, uw, dw, out,
    xr, wg, wu, wd, ag, au, hid, pb, xv, sv, av, bv, zv, ob,
    own_sem, tok_sem, tok_recv, z_sem, y_sem, c_sem, w_recv, x_sem, x_recv, a_sem, a_recv, b_sem, b_recv, zv_sem, zv_recv, out_sem,
):
    fs, tp = lax.axis_index("fs"), lax.axis_index("tp")
    z, y = lax.div(fs, ny), lax.rem(fs, ny)
    x, c = lax.div(tp, CORES), lax.rem(tp, CORES)
    near, other = flip(z, 1), 1 - c
    prim = c == lax.rem(z, 2)
    second = c != lax.rem(z, 2)
    count, width = xr.shape
    pieces, rp, ff = wg.shape[1], wg.shape[3], wg.shape[4]
    rows_in, wide = gw.shape[0], wd.shape[3]
    fp = ff // pieces
    part = count // nx
    chunks = tok_recv.shape[0]
    chunk = part // chunks
    keep = part // CORES
    scope = jax.named_scope

    def dev(z, y, x, c):
        return (z * ny + y, x * CORES + c)

    def send(src, dst, sent, got, where):
        pltpu.make_async_remote_copy(src_ref=src, dst_ref=dst, send_sem=sent, recv_sem=got, device_id=where, device_id_type=MESH).start()

    def wait(ref, sem):
        pltpu.make_async_copy(ref, ref, sem).wait()

    inside = inner(z)

    def pick(edge, middle):
        if isinstance(edge, int) and edge == middle:
            return edge
        return edge + inside * (middle - edge)

    def source(q):
        if isinstance(q, tuple):
            return pick(source(q[0]), source(q[1]))
        there = flip(z, q)
        return swap_last(there, inside) if q > 1 else there

    def number(v):
        return pick(*v) if isinstance(v, tuple) else v

    def slot(m, i, q, s):
        i, q = number(i), number(q)
        if m == DOWN:
            return wd.at[q, s, pl.ds(i * fp, fp)]
        return (wg, wu)[m].at[q, i, s]

    def mine(m, i):
        if m == DOWN:
            return dw.at[pl.ds(i * fp, fp)]
        return (gw, uw)[m].at[pl.ds(i * rp, rp)]

    def to_z(m, i, r):
        there = flip(z, r)
        q = r if r < 2 else swap_last(r, inner(there))
        send(mine(m, i), slot(m, i, q, 0), z_sem.at[m, r], w_recv.at[m, i, q, 0], dev(there, y, x, c))

    def to_y(m, i, q, src):
        for s in range(1, ny):
            send(src, slot(m, i, q, s), y_sem.at[m, s], w_recv.at[m, number(i), number(q), s], dev(z, flip(y, s), x, c))

    def to_core(m, i, q, s, src):
        send(src, slot(m, i, q, s), c_sem.at[m], w_recv.at[m, number(i), number(q), s], dev(z, y, x, other))

    def local(m, i):
        return pltpu.make_async_copy(mine(m, i), slot(m, i, 0, 0), own_sem.at[m, i])

    barrier = pltpu.get_barrier_semaphore()

    def greet(where):
        pl.semaphore_signal(barrier, inc=1, device_id=where, device_id_type=MESH)

    for r in range(1, nz):
        greet(dev(flip(z, r), y, x, c))
    for t in range(1, nx):
        greet(dev(z, y, flip(x, t), c))
    greet(dev(z, y, x, other))

    @pl.when(prim)
    def _():
        for s in range(1, ny):
            greet(dev(z, flip(y, s), x, c))
        pltpu.make_async_copy(tok, xr, tok_sem.at[nx]).start()
        for i in range(pieces):
            for m in (GATE, UP, DOWN):
                local(m, i).start()
        with scope("barrier"):
            pl.semaphore_wait(barrier, nz + nx + ny - 2)

    @pl.when(second)
    def _():
        greet(dev(near, y, x, other))
        with scope("barrier"):
            pl.semaphore_wait(barrier, nz + nx)

    def token_rows(x, k):
        return pl.ds(x * part + k * chunk, chunk)

    def to_near(k, core):
        rows = token_rows(x, k)
        send(tok.at[rows], xr.at[rows], tok_sem.at[0], tok_recv.at[k, 0], dev(near, y, x, core))

    @pl.when(prim)
    def _():
        for k in range(0, chunks, 2):
            to_near(k, c)
        for i in range(pieces):
            for m in (GATE, UP):
                to_y(m, i, 0, mine(m, i))
                for r in range(2, nz, 2):
                    to_z(m, i, r)
        for m in (GATE, UP, DOWN):
            for i in range(pieces):
                if m == DOWN:
                    to_y(m, i, 0, mine(m, i))
                to_core(m, i, 0, 0, mine(m, i))
        with scope("tokens"):
            wait(xr, tok_sem.at[nx])

    @pl.when(second)
    def _():
        for k in range(1, chunks, 2):
            to_near(k, other)
        for r in range(1, nz, 2):
            for i in range(pieces):
                for m in (GATE, UP):
                    to_z(m, i, r)

        for r in range(3, nz, 2):
            for i in range(pieces):

                @pl.when(inside == 1)
                def _():
                    to_z(DOWN, i, r)

        @pl.when(inside == 0)
        def _():
            for i in range(pieces):
                to_z(DOWN, i, 1)

        for k in range(chunks):
            rows = token_rows(x, k)
            with scope(f"tokens#k={k}"):
                wait(xr.at[rows], tok_recv.at[k, 0])
            for t in range(1, nx):
                send(xr.at[rows], xr.at[rows], tok_sem.at[t], tok_recv.at[k, t], dev(z, y, flip(x, t), c))
        with scope("tokens#x"):
            for t in range(1, nx):
                for k in range(chunks):
                    rows = token_rows(flip(x, t), k)
                    wait(xr.at[rows], tok_recv.at[k, t])
                wait(xr.at[pl.ds(x * part, part)], tok_sem.at[t])

    def normalize(t, carry):
        rows = pl.ds(pl.multiple_of(t * 32, 32), 32)
        xf = xr[rows, :].astype(jnp.float32)
        scale = lax.rsqrt(jnp.mean(xf * xf, axis=-1, keepdims=True) + 1e-06)
        xr[rows, :] = (xf * scale * gain[...]).astype(jnp.bfloat16)
        return carry

    with scope("normalize"):
        lax.fori_loop(0, count // 32, normalize, 0)

    def columns(q, i, s):
        at = (source(q) * ny + flip(y, s)) * rows_in + number(i) * rp
        return pl.ds(pl.multiple_of(at, rp), rp)

    def accumulate(group, begin=False, end=False, start=0, span=None):
        def step(t, carry):
            rows = pl.ds(pl.multiple_of(start + t * tile, tile), tile)
            left = jnp.concatenate([xr[rows, columns(q, i, s)] for q, i in group for s in range(ny)], axis=1)
            both = []
            for w, acc in ((wg, ag), (wu, au)):
                right = jnp.concatenate([w[number(q), number(i)].reshape(ny * rp, ff) for q, i in group], axis=0)
                total = jnp.dot(left, right, preferred_element_type=jnp.float32)
                if not begin:
                    total = acc[rows, :] + total
                if not end:
                    acc[rows, :] = total
                both.append(total)
            if end:
                g, u = both
                hid[rows, :] = (g / (1.0 + jnp.exp(-g)) * u).astype(jnp.bfloat16)
            return carry

        with scope("acc#" + "#".join(f"{q}={i}" for q, i in group)):
            lax.fori_loop(0, (span or count) // tile, step, 0)

    def take(m, i, q, s):
        if (q, s) == (0, 0):

            @pl.when(prim)
            def _():
                local(m, i).wait()

            @pl.when(second)
            def _():
                wait(slot(m, i, q, s), w_recv.at[m, number(i), number(q), s])

        else:
            with scope(f"take#m={m}#i={i}#q={q}#s={s}".replace(" ", "")):
                wait(slot(m, i, q, s), w_recv.at[m, number(i), number(q), s])

            @pl.when(prim)
            def _():
                if s == 0:
                    to_y(m, i, q, slot(m, i, q, s))
                to_core(m, i, q, s, slot(m, i, q, s))

    def take_both(i, q, rows):
        for s in rows:
            for m in (GATE, UP):
                take(m, i, q, s)

    def take_down(q, rows):
        for s in rows:
            for i in range(pieces):
                take(DOWN, i, q, s)

    here, away = range(1), range(1, ny)
    early, late = list(range(2, nz, 2)), [1] + list(range(3, nz, 2))
    every = range(pieces)
    for i in every:
        take_both(i, 0, range(ny))
    accumulate([(0, i) for i in every], begin=True)
    steps = [
        ((q0, q1), (i0, i1))
        for (q0, i0), (q1, i1) in zip([(q, i) for q in late for i in every], [(q, i) for i in every for q in late])
    ]

    def pass_on(n):
        if n < len(steps):
            q, i = steps[n]
            take_both(i, q, here)

    def down_to_z(place):
        @pl.when(prim & (inside == place))
        def _():
            for k in every:
                for r in range(2, nz, 2):
                    to_z(DOWN, k, r)

        @pl.when(second & (inside == place))
        def _():
            for k in every:
                for r in [1] if place else range(3, nz, 2):
                    to_z(DOWN, k, r)

    for q in early:
        for i in every:
            take_both(i, q, here)
    pass_on(0)
    for q in early:
        for i in every:
            take_both(i, q, away)
    pass_on(1)
    for q in early:
        accumulate([(q, k) for k in every])
    pass_on(2)
    group = []
    for n, (q, i) in enumerate(steps):
        last = n == len(steps) - 1
        if last:
            down_to_z(0)
        take_both(i, q, away)
        pass_on(n + 3)
        if n + 4 == max(len(steps), 4):
            down_to_z(1)
        group.append((q, i))
        if not last and (n == len(steps) - 2 or n % 2):
            accumulate(group)
            group = []

    def at(q, s):
        return q * ny + s

    parts = [flip(x, t) for t in range(1, nx)] + [x]
    subs = (other, c)
    straight = early[:1]

    def sub_rows(x, k):
        return pl.ds(pl.multiple_of(x * part + k * keep, keep), keep)

    def to_x(j, t):
        there = flip(x, t)
        for h, k in enumerate(subs):
            send(pb.at[j, sub_rows(there, k)], xv.at[t - 1, j, h], x_sem.at[t], x_recv.at[t, j, h], dev(z, y, there, c))

    def partial(q, s, head=None):
        j = at(q, s)
        for t, p in enumerate(parts):
            start = p * part
            if head:
                head(start)

            def step(t, carry):
                rows = pl.ds(pl.multiple_of(start + t * tile, tile), tile)
                pb[j, rows, :] = jnp.dot(hid[rows, :], wd[q, s], preferred_element_type=jnp.float32).astype(jnp.bfloat16)
                return carry

            with scope(f"part#q={q}#s={s}"):
                lax.fori_loop(0, part // tile, step, 0)
            if q not in straight and t + 1 < nx:
                to_x(j, t + 1)
            if q in straight:

                @pl.when(second)
                def _():
                    rows = pl.ds(pl.multiple_of(start, part), part)
                    send(pb.at[j, rows], zv.at[s, rows], zv_sem, zv_recv.at[s, t], dev(near, y, x, c))

    def gather_z(q, s):
        j = at(q, s)

        @pl.when(prim)
        def _():
            for t, p in enumerate(parts):
                rows = pl.ds(pl.multiple_of(p * part, part), part)
                with scope(f"zwait#q={q}#s={s}"):
                    wait(zv.at[s, rows], zv_recv.at[s, t])
                pb[j, rows, :] = (pb[j, rows, :].astype(jnp.float32) + zv[s, rows, :].astype(jnp.float32)).astype(jnp.bfloat16)
                if t + 1 < nx:
                    to_x(j, t + 1)

    def added(j, h, k):
        total = pb[j, sub_rows(x, k), :].astype(jnp.float32)
        for t in range(1, nx):
            with scope(f"xwait#j={j}"):
                wait(xv.at[t - 1, j, h], x_recv.at[t, j, h])
            total = total + xv[t - 1, j, h].astype(jnp.float32)
        return total.astype(jnp.bfloat16)

    def gather_x(q, s):
        j = at(q, s)
        if q in straight:

            @pl.when(prim)
            def _():
                for h, k in enumerate(subs):
                    sv[j, h] = added(j, h, k)
                    if h == 0:
                        send(sv.at[j, h], av.at[j], a_sem, a_recv.at[j], dev(z, y, x, other))

            return
        there = at(1 - q if q < 2 else q, s)
        for h, k in enumerate(subs):
            sv[j, h] = added(j, h, k)
            if h == 0:

                @pl.when(prim)
                def _():
                    send(sv.at[j, h], av.at[j], a_sem, a_recv.at[j], dev(z, y, x, other))

            @pl.when(second)
            def _():
                send(sv.at[j, h], bv.at[there], b_sem.at[h], b_recv.at[there], dev(near, y, x, k))

    def finish(q, s):
        j = at(q, s)
        to = pl.ds(pl.multiple_of((source(q) * ny + flip(y, s)) * wide, wide), wide)
        if q not in straight:
            with scope(f"bwait#q={q}#s={s}"):
                wait(bv.at[j], b_recv.at[j])

        def put(value):
            if q not in straight:
                value = (value.astype(jnp.float32) + bv[j].astype(jnp.float32)).astype(jnp.bfloat16)
            ob[j] = value

        @pl.when(prim)
        def _():
            put(sv[j, 1])

        @pl.when(second)
        def _():
            wait(av.at[j], a_recv.at[j])
            put(av[j])

        pltpu.make_async_copy(ob.at[j], out.at[:, to], out_sem).start()

    order = [(0, s) for s in range(ny)]
    order += [(q, 0) for q in early[:1]] + [(1, 0)]
    order += [(q, s) for q in early[:1] for s in away]
    order += [(q, 0) for q in late[1:] + early[1:]]
    order += [(q, s) for q in late + early[1:] for s in away]
    ahead = {1: [(q, 0) for q in early[:1]], ny: [(1, 0)]}
    if early:
        ahead[order.index((early[0], ny - 1)) + 1] = [(q, 0) for q in late[1:]]
    taken = []
    lag, behind = 3, 5
    finishes, sums, adds = {}, {}, {}
    for n, (q, s) in enumerate(order):
        extra = 0
        if q in straight:
            sums.setdefault(n + 3, []).append((q, s))
            extra = 2
        adds.setdefault(n + lag + extra, []).append((q, s))
        n = max(n, order.index((1 - q if q < 2 else q, s)))
        finishes.setdefault(n + behind, []).append((q, s))
    for n in range(len(order) + behind):
        for q, s in sums.get(n, ()):
            gather_z(q, s)
        for q, s in ahead.get(n, []) + order[n : n + 1]:
            if (q, s) not in taken:
                taken.append((q, s))
                take_down(q, range(s, s + 1))
        if n == 0:
            partial(*order[0], head=lambda start: accumulate(group, end=True, start=start, span=part))
        elif 0 < n < len(order):
            partial(*order[n])
        for q, s in adds.get(n, ()):
            gather_x(q, s)
        for q, s in finishes.get(n, ()):
            finish(q, s)

    wait(ob, out_sem)
    wait(xr.at[pl.ds(0, part // 2)], tok_sem.at[0])
    n_across = xv.shape[1] - ny * len(straight)

    def block(m):
        return wd.at[0, 0] if m == DOWN else (wg, wu)[m].at[0, :, 0]

    @pl.when(prim)
    def _():
        for m, whole, line in ((GATE, wg, wg.at[:, :, 0]), (UP, wu, wu.at[:, :, 0]), (DOWN, wd, wd.at[:, 0])):
            for r in range(2, nz, 2):
                wait(block(m), z_sem.at[m, r])
            for s in range(1, ny):
                wait(line, y_sem.at[m, s])
            wait(whole, c_sem.at[m])
        for t in range(1, nx):
            wait(xv.at[t - 1], x_sem.at[t])
        wait(av, a_sem)

    @pl.when(second)
    def _():
        for m in (GATE, UP, DOWN):
            for r in range(1, nz, 2):
                wait(block(m), z_sem.at[m, r])
        for t in range(1, nx):
            wait(xv.at[t - 1, pl.ds(0, n_across)], x_sem.at[t])
        for k in range(CORES):
            wait(bv.at[pl.ds(0, n_across)], b_sem.at[k])
        if straight:
            wait(zv, zv_sem)


def make_per_device(n, n_tp):
    nz, ny = fs_grid(n)
    nx = n_tp // CORES

    def per_device(tokens, norm_gain, gate_weight, up_weight, down_weight):
        count, width = tokens.shape
        rows, ff = gate_weight.shape
        wide = down_weight.shape[1]
        pieces = max(rows // 128, 1)
        keep = count // n_tp
        part = count // nx
        chunks = 8
        tile = min(256, count)
        bf16, f32 = jnp.bfloat16, jnp.float32
        dma = pltpu.SemaphoreType.DMA
        vmem = pl.BlockSpec(memory_space=pltpu.VMEM)
        hbm = pl.BlockSpec(memory_space=pl.ANY)
        return pl.pallas_call(
            functools.partial(kernel, nz, ny, nx, tile),
            name="gated_block",
            out_shape=jax.ShapeDtypeStruct((keep, width), bf16),
            in_specs=[hbm, vmem, hbm, hbm, hbm],
            out_specs=hbm,
            scratch_shapes=[
                pltpu.VMEM((count, width), bf16),
                pltpu.VMEM((nz, pieces, ny, rows // pieces, ff), bf16),
                pltpu.VMEM((nz, pieces, ny, rows // pieces, ff), bf16),
                pltpu.VMEM((nz, ny, ff, wide), bf16),
                pltpu.VMEM((count, ff), f32),
                pltpu.VMEM((count, ff), f32),
                pltpu.VMEM((count, ff), bf16),
                pltpu.VMEM((n, count, wide), bf16),
                pltpu.VMEM((nx - 1, n, CORES, keep, wide), bf16),
                pltpu.VMEM((n, CORES, keep, wide), bf16),
                pltpu.VMEM((n, keep, wide), bf16),
                pltpu.VMEM((n, keep, wide), bf16),
                pltpu.VMEM((ny, count, wide), bf16),
                pltpu.VMEM((n, keep, wide), bf16),
                dma((3, pieces)),
                dma((nx + 1,)),
                dma((chunks, nx)),
                dma((3, nz)),
                dma((3, ny)),
                dma((3,)),
                dma((3, pieces, nz, ny)),
                dma((nx,)),
                dma((nx, n, CORES)),
                dma,
                dma((n,)),
                dma((CORES,)),
                dma((n,)),
                dma,
                dma((ny, nx)),
                dma,
            ],
            compiler_params=pltpu.CompilerParams(collective_id=0, has_side_effects=True, vmem_limit_bytes=67043328),
        )(tokens, norm_gain.reshape(1, width), gate_weight, up_weight, down_weight)

    return per_device


def solution(mesh):
    placed = (P("fs", None), P(), P("fs", "tp"), P("fs", "tp"), P("tp", "fs"))
    return jax.shard_map(
        make_per_device(mesh.shape["fs"], mesh.shape["tp"]),
        mesh=mesh, in_specs=placed, out_specs=P(("fs", "tp"), None), check_vma=False,
    )
```

```python
import functools

import jax
import jax.numpy as jnp
from jax import lax
from jax.experimental import pallas as pl
from jax.experimental.pallas import tpu as pltpu
from jax.sharding import PartitionSpec as P

MESH = pl.DeviceIdType.MESH
CORES = 2
GATE, UP, DOWN = 0, 1, 2


def fs_grid(n):
    ny = 1
    while ny * ny * 4 <= n:
        ny *= 2
    return n // ny, ny


def flip(v, bits):
    bit = 1
    while bit <= bits:
        if bits & bit:
            v = v + bit - 2 * bit * lax.rem(lax.div(v, bit), 2)
        bit *= 2
    return v


def inner(z):
    return lax.rem(lax.rem(z, 2) + lax.rem(lax.div(z, 2), 2), 2)


def swap_last(v, on):
    return v + on * (1 - 2 * lax.rem(v, 2))


def kernel(
    nz, ny, nx, tile, tok, gain, gw, uw, dw, out,
    xr, wg, wu, wd, ag, au, hid, pb, xv, sv, av, bv, zv, ob,
    own_sem, tok_sem, tok_recv, z_sem, y_sem, c_sem, w_recv, x_sem, x_recv, a_sem, a_recv, b_sem, b_recv, zv_sem, zv_recv, out_sem,
):
    fs, tp = lax.axis_index("fs"), lax.axis_index("tp")
    z, y = lax.div(fs, ny), lax.rem(fs, ny)
    x, c = lax.div(tp, CORES), lax.rem(tp, CORES)
    near, other = flip(z, 1), 1 - c
    prim = c == lax.rem(z, 2)
    second = c != lax.rem(z, 2)
    count, width = xr.shape
    pieces, rp, ff = wg.shape[1], wg.shape[3], wg.shape[4]
    rows_in, wide = gw.shape[0], wd.shape[3]
    fp = ff // pieces
    part = count // nx
    chunks = tok_recv.shape[0]
    chunk = part // chunks
    keep = part // CORES
    scope = jax.named_scope

    def dev(z, y, x, c):
        return (z * ny + y, x * CORES + c)

    def send(src, dst, sent, got, where):
        pltpu.make_async_remote_copy(src_ref=src, dst_ref=dst, send_sem=sent, recv_sem=got, device_id=where, device_id_type=MESH).start()

    def wait(ref, sem):
        pltpu.make_async_copy(ref, ref, sem).wait()

    inside = inner(z)

    def pick(edge, middle):
        if isinstance(edge, int) and edge == middle:
            return edge
        return edge + inside * (middle - edge)

    def source(q):
        if isinstance(q, tuple):
            return pick(source(q[0]), source(q[1]))
        there = flip(z, q)
        return swap_last(there, inside) if q > 1 else there

    def number(v):
        return pick(*v) if isinstance(v, tuple) else v

    cuts = w_recv.shape[4]
    cut = rp // cuts

    def slot(m, i, q, s, h):
        i, q = number(i), number(q)
        if m == DOWN:
            return wd.at[q, s, pl.ds(i * fp, fp)]
        return (wg, wu)[m].at[q, i, s, pl.ds(h * cut, cut)]

    def mine(m, i, h):
        if m == DOWN:
            return dw.at[pl.ds(i * fp, fp)]
        return (gw, uw)[m].at[pl.ds(i * rp + h * cut, cut)]

    def halves(m):
        return range(1 if m == DOWN else cuts)

    def to_z(m, i, r):
        there = flip(z, r)
        q = r if r < 2 else swap_last(r, inner(there))
        for h in halves(m):
            send(mine(m, i, h), slot(m, i, q, 0, h), z_sem.at[m, r], w_recv.at[m, i, q, 0, h], dev(there, y, x, c))

    def to_y(m, i, q, h, src):
        for s in range(1, ny):
            got = w_recv.at[m, number(i), number(q), s, h]
            send(src, slot(m, i, q, s, h), y_sem.at[m, s], got, dev(z, flip(y, s), x, c))

    def to_core(m, i, q, s, h, src):
        got = w_recv.at[m, number(i), number(q), s, h]
        send(src, slot(m, i, q, s, h), c_sem.at[m], got, dev(z, y, x, other))

    def local(m, i, h):
        return pltpu.make_async_copy(mine(m, i, h), slot(m, i, 0, 0, h), own_sem.at[m, i, h])

    barrier = pltpu.get_barrier_semaphore()

    def greet(where):
        pl.semaphore_signal(barrier, inc=1, device_id=where, device_id_type=MESH)

    for r in range(1, nz):
        greet(dev(flip(z, r), y, x, c))
    for t in range(1, nx):
        greet(dev(z, y, flip(x, t), c))
    greet(dev(z, y, x, other))

    @pl.when(prim)
    def _():
        for s in range(1, ny):
            greet(dev(z, flip(y, s), x, c))
        pltpu.make_async_copy(tok, xr, tok_sem.at[nx]).start()
        for i in range(pieces):
            for m in (GATE, UP, DOWN):
                for h in halves(m):
                    local(m, i, h).start()
        with scope("barrier"):
            pl.semaphore_wait(barrier, nz + nx + ny - 2)

    @pl.when(second)
    def _():
        greet(dev(near, y, x, other))
        with scope("barrier"):
            pl.semaphore_wait(barrier, nz + nx)

    def token_rows(x, k):
        return pl.ds(x * part + k * chunk, chunk)

    def to_near(k, core):
        rows = token_rows(x, k)
        send(tok.at[rows], xr.at[rows], tok_sem.at[0], tok_recv.at[k, 0], dev(near, y, x, core))

    @pl.when(prim)
    def _():
        for k in range(0, chunks, 2):
            to_near(k, c)
        for i in range(pieces):
            for m in (GATE, UP):
                for h in halves(m):
                    to_y(m, i, 0, h, mine(m, i, h))
                for r in range(2, nz, 2):
                    to_z(m, i, r)
        for m in (GATE, UP, DOWN):
            for i in range(pieces):
                for h in halves(m):
                    if m == DOWN:
                        to_y(m, i, 0, h, mine(m, i, h))
                    to_core(m, i, 0, 0, h, mine(m, i, h))
        with scope("tokens"):
            wait(xr, tok_sem.at[nx])

    @pl.when(second)
    def _():
        to_z(GATE, 0, 1)
        to_z(UP, 0, 1)
        for k in range(1, chunks, 2):
            to_near(k, other)
        for r in range(1, nz, 2):
            for i in range(1 if r == 1 else 0, pieces):
                for m in (GATE, UP):
                    to_z(m, i, r)

        for r in range(3, nz, 2):
            for i in range(pieces):

                @pl.when(inside == 1)
                def _():
                    to_z(DOWN, i, r)

        @pl.when(inside == 0)
        def _():
            for i in range(pieces):
                to_z(DOWN, i, 1)

        for k in range(chunks):
            rows = token_rows(x, k)
            with scope(f"tokens#k={k}"):
                wait(xr.at[rows], tok_recv.at[k, 0])
            for t in range(1, nx):
                send(xr.at[rows], xr.at[rows], tok_sem.at[t], tok_recv.at[k, t], dev(z, y, flip(x, t), c))
        with scope("tokens#x"):
            for t in range(1, nx):
                for k in range(chunks):
                    rows = token_rows(flip(x, t), k)
                    wait(xr.at[rows], tok_recv.at[k, t])
                wait(xr.at[pl.ds(x * part, part)], tok_sem.at[t])

    def normalize(t, carry):
        rows = pl.ds(pl.multiple_of(t * 32, 32), 32)
        xf = xr[rows, :].astype(jnp.float32)
        scale = lax.rsqrt(jnp.mean(xf * xf, axis=-1, keepdims=True) + 1e-06)
        xr[rows, :] = (xf * scale * gain[...]).astype(jnp.bfloat16)
        return carry

    with scope("normalize"):
        lax.fori_loop(0, count // 32, normalize, 0)

    def columns(q, i, s):
        at = (source(q) * ny + flip(y, s)) * rows_in + number(i) * rp
        return pl.ds(pl.multiple_of(at, rp), rp)

    def accumulate(group, begin=False, end=False, start=0, span=None):
        def step(t, carry):
            rows = pl.ds(pl.multiple_of(start + t * tile, tile), tile)
            left = jnp.concatenate([xr[rows, columns(q, i, s)] for q, i in group for s in range(ny)], axis=1)
            both = []
            for w, acc in ((wg, ag), (wu, au)):
                right = jnp.concatenate([w[number(q), number(i)].reshape(ny * rp, ff) for q, i in group], axis=0)
                total = jnp.dot(left, right, preferred_element_type=jnp.float32)
                if not begin:
                    total = acc[rows, :] + total
                if not end:
                    acc[rows, :] = total
                both.append(total)
            if end:
                g, u = both
                hid[rows, :] = (g / (1.0 + jnp.exp(-g)) * u).astype(jnp.bfloat16)
            return carry

        with scope("acc#" + "#".join(f"{q}={i}" for q, i in group)):
            if span == tile:
                step(0, 0)
            else:
                lax.fori_loop(0, (span or count) // tile, step, 0)

    pending = []

    def enqueue(group, begin=False):
        for t in range(count // tile):
            pending.append(functools.partial(accumulate, group, begin=begin, start=t * tile, span=tile))

    def drain():
        while pending:
            pending.pop(0)()

    def take(m, i, q, s):
        for h in halves(m):
            if (q, s) == (0, 0):

                @pl.when(prim)
                def _():
                    local(m, i, h).wait()

                @pl.when(second)
                def _():
                    wait(slot(m, i, q, s, h), w_recv.at[m, i, q, s, h])

            else:
                with scope(f"take#m={m}#i={i}#q={q}#s={s}#h={h}".replace(" ", "")):
                    wait(slot(m, i, q, s, h), w_recv.at[m, number(i), number(q), s, h])

                @pl.when(prim)
                def _():
                    if s == 0:
                        to_y(m, i, q, h, slot(m, i, q, s, h))
                    to_core(m, i, q, s, h, slot(m, i, q, s, h))

            if pending:
                pending.pop(0)()

    def take_both(i, q, rows):
        for s in rows:
            for m in (GATE, UP):
                take(m, i, q, s)

    def take_down(q, rows):
        for s in rows:
            for i in range(pieces):
                take(DOWN, i, q, s)

    here, away = range(1), range(1, ny)
    early, late = list(range(2, nz, 2)), [1] + list(range(3, nz, 2))
    every = range(pieces)
    for i in every:
        take_both(i, 0, range(ny))
    enqueue([(0, i) for i in every], begin=True)
    drain()
    steps = [
        ((q0, q1), (i0, i1))
        for (q0, i0), (q1, i1) in zip([(q, i) for q in late for i in every], [(q, i) for i in every for q in late])
    ]

    def pass_on(n):
        if n < len(steps):
            q, i = steps[n]
            take_both(i, q, here)

    def down_to_z(place, core):
        @pl.when((prim if core == 0 else second) & (inside == place))
        def _():
            for k in every:
                for r in range(2, nz, 2) if core == 0 else [1] if place else range(3, nz, 2):
                    to_z(DOWN, k, r)

    for q in early:
        take_both(0, q, here)
    pass_on(0)
    for q in early:
        for i in every[1:]:
            take_both(i, q, here)
    for m in (GATE, UP):
        for q in early:
            for i in every if m == GATE else every[-1:]:
                for s in away:
                    take(m, i, q, s)
                    if m == GATE and i < pieces - 1:
                        take(UP, i, q, s)
        if len(steps) > 1:
            take(m, steps[1][1], steps[1][0], 0)
    for q in early:
        enqueue([(q, i) for i in every])
    pass_on(2)
    group = []
    for n, (q, i) in enumerate(steps):
        last = n == len(steps) - 1
        if last:
            drain()
        take_both(i, q, away)
        group.append((q, i))
        if not last and (n == len(steps) - 2 or n % 2):
            enqueue(group)
            group = []
        if n == min(1, len(steps) - 1):
            down_to_z(1, 0)
            down_to_z(1, 1)
        if n > 0:
            pass_on(n + 2)

    def at(q, s):
        return q * ny + s

    parts = [flip(x, t) for t in range(1, nx)] + [x]
    subs = (other, c)
    straight = late[1:2]

    def sub_rows(x, k):
        return pl.ds(pl.multiple_of(x * part + k * keep, keep), keep)

    def to_x(j, t, h):
        there = flip(x, t)
        rows = sub_rows(there, subs[h])
        send(pb.at[j, rows], xv.at[t - 1, j, h], x_sem.at[t], x_recv.at[t, j, h], dev(z, y, there, c))

    def partial(q, s, head=None):
        j = at(q, s)
        for t, p in enumerate(parts):
            for h, k in enumerate(subs):
                start = p * part + k * keep
                if head:
                    head(start)
                    if (t, h) == (nx - 1, 0):
                        down_to_z(0, 0)

                def step(n, carry):
                    rows = pl.ds(pl.multiple_of(start + n * tile, tile), tile)
                    pb[j, rows, :] = jnp.dot(hid[rows, :], wd[q, s], preferred_element_type=jnp.float32).astype(jnp.bfloat16)
                    return carry

                with scope(f"part#q={q}#s={s}"):
                    lax.fori_loop(0, keep // tile, step, 0)
                if q not in straight and t + 1 < nx:
                    to_x(j, t + 1, h)
                if q in straight:

                    @pl.when(second)
                    def _():
                        rows = pl.ds(pl.multiple_of(start, keep), keep)
                        send(pb.at[j, rows], zv.at[s, rows], zv_sem, zv_recv.at[s, t, h], dev(near, y, x, c))

    def gather_z(q, s):
        j = at(q, s)

        @pl.when(prim)
        def _():
            for t, p in enumerate(parts):
                for h, k in enumerate(subs):
                    rows = sub_rows(p, k)
                    with scope(f"zwait#q={q}#s={s}"):
                        wait(zv.at[s, rows], zv_recv.at[s, t, h])
                    pb[j, rows, :] = (pb[j, rows, :].astype(jnp.float32) + zv[s, rows, :].astype(jnp.float32)).astype(jnp.bfloat16)
                    if t + 1 < nx:
                        to_x(j, t + 1, h)

    def added(j, h, k):
        total = pb[j, sub_rows(x, k), :].astype(jnp.float32)
        for t in range(1, nx):
            with scope(f"xwait#j={j}"):
                wait(xv.at[t - 1, j, h], x_recv.at[t, j, h])
            total = total + xv[t - 1, j, h].astype(jnp.float32)
        return total.astype(jnp.bfloat16)

    def gather_x(q, s):
        j = at(q, s)
        if q in straight:

            @pl.when(prim)
            def _():
                for h, k in enumerate(subs):
                    sv[j, h] = added(j, h, k)
                    if h == 0:
                        send(sv.at[j, h], av.at[j], a_sem, a_recv.at[j], dev(z, y, x, other))

            return
        there = at(1 - q if q < 2 else q, s)
        for h, k in enumerate(subs):
            sv[j, h] = added(j, h, k)
            if h == 0:

                @pl.when(prim)
                def _():
                    send(sv.at[j, h], av.at[j], a_sem, a_recv.at[j], dev(z, y, x, other))

            @pl.when(second)
            def _():
                send(sv.at[j, h], bv.at[there], b_sem.at[h], b_recv.at[there], dev(near, y, x, k))

    def finish(q, s):
        j = at(q, s)
        to = pl.ds(pl.multiple_of((source(q) * ny + flip(y, s)) * wide, wide), wide)
        if q not in straight:
            with scope(f"bwait#q={q}#s={s}"):
                wait(bv.at[j], b_recv.at[j])

        def put(value):
            if q not in straight:
                value = (value.astype(jnp.float32) + bv[j].astype(jnp.float32)).astype(jnp.bfloat16)
            ob[j] = value

        @pl.when(prim)
        def _():
            put(sv[j, 1])

        @pl.when(second)
        def _():
            wait(av.at[j], a_recv.at[j])
            put(av[j])

        pltpu.make_async_copy(ob.at[j], out.at[:, to], out_sem).start()

    order = [(0, s) for s in range(ny)]
    order += [(q, 0) for q in early[:1]] + [(1, 0)]
    order += [(q, s) for q in early[:1] for s in away]
    order += [(q, 0) for q in late[1:] + early[1:]]
    order += [(q, s) for q in late + early[1:] for s in away]
    ahead = {1: [(q, 0) for q in early[:1]], ny: [(1, 0)]}
    taken = []
    lag, behind = 3, 6
    finishes, sums, adds = {}, {}, {}
    for n, (q, s) in enumerate(order):
        extra = 0
        if q in straight:
            sums.setdefault(n + 3, []).append((q, s))
            extra = 2
        adds.setdefault(n + lag + extra, []).append((q, s))
        n = max(n, order.index((1 - q if q < 2 else q, s)))
        finishes.setdefault(max(n + behind, len(order) + 2), []).append((q, s))
    for n in range(len(order) + behind):
        for q, s in sums.get(n, ()):
            gather_z(q, s)
        for q, s in ahead.get(n, []) + order[n : n + 1]:
            if (q, s) not in taken:
                taken.append((q, s))
                take_down(q, range(s, s + 1))
        if n == 0:
            partial(*order[0], head=lambda start: accumulate(group, end=True, start=start, span=keep))
            down_to_z(0, 1)
        elif 0 < n < len(order):
            partial(*order[n])
        for q, s in adds.get(n, ()):
            gather_x(q, s)
        for q, s in finishes.get(n, ()):
            finish(q, s)

    wait(ob, out_sem)
    wait(xr.at[pl.ds(0, part // 2)], tok_sem.at[0])
    n_across = xv.shape[1] - ny * len(straight)

    def block(m):
        return wd.at[0, 0] if m == DOWN else (wg, wu)[m].at[0, :, 0]

    @pl.when(prim)
    def _():
        for m, whole, line in ((GATE, wg, wg.at[:, :, 0]), (UP, wu, wu.at[:, :, 0]), (DOWN, wd, wd.at[:, 0])):
            for r in range(2, nz, 2):
                wait(block(m), z_sem.at[m, r])
            for s in range(1, ny):
                wait(line, y_sem.at[m, s])
            wait(whole, c_sem.at[m])
        for t in range(1, nx):
            wait(xv.at[t - 1], x_sem.at[t])
        wait(av, a_sem)

    @pl.when(second)
    def _():
        for m in (GATE, UP, DOWN):
            for r in range(1, nz, 2):
                wait(block(m), z_sem.at[m, r])
        for t in range(1, nx):
            wait(xv.at[t - 1, pl.ds(0, n_across)], x_sem.at[t])
        for k in range(CORES):
            wait(bv.at[pl.ds(0, n_across)], b_sem.at[k])
        if straight:
            wait(zv, zv_sem)


def make_per_device(n, n_tp):
    nz, ny = fs_grid(n)
    nx = n_tp // CORES

    def per_device(tokens, norm_gain, gate_weight, up_weight, down_weight):
        count, width = tokens.shape
        rows, ff = gate_weight.shape
        wide = down_weight.shape[1]
        pieces = max(rows // 128, 1)
        keep = count // n_tp
        part = count // nx
        chunks, cuts = 8, 2
        tile = min(256, keep)
        bf16, f32 = jnp.bfloat16, jnp.float32
        dma = pltpu.SemaphoreType.DMA
        vmem = pl.BlockSpec(memory_space=pltpu.VMEM)
        hbm = pl.BlockSpec(memory_space=pl.ANY)
        return pl.pallas_call(
            functools.partial(kernel, nz, ny, nx, tile),
            name="gated_block",
            out_shape=jax.ShapeDtypeStruct((keep, width), bf16),
            in_specs=[hbm, vmem, hbm, hbm, hbm],
            out_specs=hbm,
            scratch_shapes=[
                pltpu.VMEM((count, width), bf16),
                pltpu.VMEM((nz, pieces, ny, rows // pieces, ff), bf16),
                pltpu.VMEM((nz, pieces, ny, rows // pieces, ff), bf16),
                pltpu.VMEM((nz, ny, ff, wide), bf16),
                pltpu.VMEM((count, ff), f32),
                pltpu.VMEM((count, ff), f32),
                pltpu.VMEM((count, ff), bf16),
                pltpu.VMEM((n, count, wide), bf16),
                pltpu.VMEM((nx - 1, n, CORES, keep, wide), bf16),
                pltpu.VMEM((n, CORES, keep, wide), bf16),
                pltpu.VMEM((n, keep, wide), bf16),
                pltpu.VMEM((n, keep, wide), bf16),
                pltpu.VMEM((ny, count, wide), bf16),
                pltpu.VMEM((n, keep, wide), bf16),
                dma((3, pieces, cuts)),
                dma((nx + 1,)),
                dma((chunks, nx)),
                dma((3, nz)),
                dma((3, ny)),
                dma((3,)),
                dma((3, pieces, nz, ny, cuts)),
                dma((nx,)),
                dma((nx, n, CORES)),
                dma,
                dma((n,)),
                dma((CORES,)),
                dma((n,)),
                dma,
                dma((ny, nx, CORES)),
                dma,
            ],
            compiler_params=pltpu.CompilerParams(collective_id=0, has_side_effects=True, vmem_limit_bytes=67043328),
        )(tokens, norm_gain.reshape(1, width), gate_weight, up_weight, down_weight)

    return per_device


def solution(mesh):
    placed = (P("fs", None), P(), P("fs", "tp"), P("fs", "tp"), P("tp", "fs"))
    return jax.shard_map(
        make_per_device(mesh.shape["fs"], mesh.shape["tp"]),
        mesh=mesh, in_specs=placed, out_specs=P(("fs", "tp"), None), check_vma=False,
    )
```
